32 devices in a mesh: kv: 8 (over z, y), tp: 4 (over x, core).
Axes of the slice: x: 2, y: 2, z: 4, core: 2. Of those that a mesh axis runs over, the one named last changes fastest.
Arguments:
- tokens: bfloat16 [160, 4096], P(None, 'kv'), may hold values from -40 to 40
- input_norm_gain: float32 [4096], P('kv'), may hold values from 0.1 to 1.9
- input_matrix: bfloat16 [4096, 4096], P('kv', 'tp'), may hold values from -0.09375 to 0.09375
- gate_matrix: bfloat16 [4096, 4096], P('kv', 'tp'), may hold values from -0.09375 to 0.09375
- write_matrix: bfloat16 [4096, 1024], P('kv', 'tp'), may hold values from -0.09375 to 0.09375
- read_matrix: bfloat16 [4096, 1024], P('kv', 'tp'), may hold values from -0.09375 to 0.09375
- step_matrix: bfloat16 [4096, 64], replicated, may hold values from -0.09375 to 0.09375
- input_kernel: float32 [4, 4096], P(None, 'tp'), may hold values from -3 to 3
- write_kernel: float32 [4, 1024], P(None, 'tp'), may hold values from -3 to 3
- read_kernel: float32 [4, 1024], P(None, 'tp'), may hold values from -3 to 3
- step_size_bias: float32 [64], P('tp'), may hold values from -6 to 1
- head_decay_logs: float32 [64], P('tp'), may hold values from 0 to 2.77
- bypass_scale: float32 [64], P('tp'), may hold values from 0.5 to 1.5
- extra_decay_logs: float32 [160, 64], P('kv', 'tp'), may hold values from -0.7 to 0, as said below
- output_norm_gain: float32 [4096], P('tp'), may hold values from 0.1 to 1.9
- output_matrix: bfloat16 [4096, 4096], P('tp', 'kv'), may hold values from -0.09375 to 0.09375
- cached_state_history: float32 [32, 6, 64, 64, 128], P('kv', None, 'tp'), may hold values from -2 to 2
- cached_input_rows: bfloat16 [32, 8, 4096], P('kv', None, 'tp'), may hold values from -6 to 6
- cached_write_rows: bfloat16 [32, 8, 1024], P('kv', None, 'tp'), may hold values from -6 to 6
- cached_read_rows: bfloat16 [32, 8, 1024], P('kv', None, 'tp'), may hold values from -6 to 6
- accepted: int32 [32], P('kv'), may hold values from 0 to 5
Outputs:
- mixer_out: bfloat16 [160, 4096], P('tp', 'kv')
- next_states: float32 [32, 6, 64, 64, 128], P('kv', None, 'tp')
- next_input: bfloat16 [32, 8, 4096], P('kv', None, 'tp')
- next_write: bfloat16 [32, 8, 1024], P('kv', None, 'tp')
- next_read: bfloat16 [32, 8, 1024], P('kv', None, 'tp')
The draws below stay inside these ranges and needn't reach their ends.
Inputs may be any that keep to these rules, and one draw needn't show every extreme that they name: `extra_decay_logs`: zero at most tokens and heads.
All inputs are finite; a program needn't handle non-finite values.
Results may differ from the reference program's by a relative error of at most 0.03.
Values may be sent and summed in bfloat16 or wider, within the bound.
A program may use at most 64 MiB of HBM per device.

```python
import math
import jax
import jax.numpy as jnp
from jax import lax

D = 4096
HEAD_TOTAL = 64
P_SIZE = 64
N = 128
G = 8
TAPS = 4
DRAFT_TOKENS = 5
SEQUENCE_TOTAL = 32
TOKENS = 160
N_TP = 4


def draw_tokens(key, part):
    first, second, third = jax.random.split(jax.random.fold_in(key, 11), 3)
    column = jnp.arange(D, dtype=jnp.float32)
    column_scale = jnp.exp(math.log(3.0) * column / max(D - 1, 1)) * jnp.exp(jax.random.uniform(second, (D,), jnp.float32, -0.35, 0.35))
    base = jax.random.normal(first, (TOKENS, D), jnp.float32)
    row_scale = jnp.exp(jax.random.uniform(third, (TOKENS, 1), jnp.float32, math.log(0.3), math.log(3.0)))
    values = jnp.clip(base * row_scale * column_scale[None, :], -40.0, 40.0)
    return values.astype(jnp.bfloat16)


def draw_extra_decay_logs(key, part):
    first, second = jax.random.split(jax.random.fold_in(key, 23), 2)
    struck = jax.random.randint(first, (TOKENS, HEAD_TOTAL), 0, 4) == 0
    depth = jax.random.uniform(second, (TOKENS, HEAD_TOTAL), jnp.float32, -0.5, -0.22)
    return jnp.where(struck, depth, 0.0).astype(jnp.float32)


def touch_ends(result, key, low, high):
    longest = result.shape.index(max(result.shape))
    spots = []
    for shift in (0, 1):
        where = [jax.random.randint(jax.random.fold_in(key, axis), (), 0, length) for axis, length in enumerate(result.shape)]
        where[longest] = (where[longest] + shift) % result.shape[longest]
        spots.append(tuple(where))
    return result.at[spots[0]].set(low).at[spots[1]].set(high)


def block_levels(rng, dims, cuts, low, top_value):
    gain = 1.0
    for dim, parts in cuts:
        draws = jax.random.uniform(jax.random.fold_in(jax.random.fold_in(rng, 6), dim), (parts,), jnp.float32, low / len(cuts), top_value / len(cuts))
        gain = gain * jnp.repeat(jnp.exp(draws), dims[dim] // parts).reshape((-1,) + (1,) * (len(dims) - 1 - dim))
    return gain


def gaussian(own_key, extent, width, reach, cuts=(), kind=jnp.bfloat16):
    values = jax.random.normal(own_key, extent, jnp.float32) * width
    if len(cuts) > 0:
        values = block_levels(own_key, extent, cuts, -0.22, 0.18) * values
    return jnp.clip(values, min=-reach, max=reach).astype(kind)


def setup_inputs(seed: int = 0) -> dict:
    key_list = jax.random.split(jax.random.key(seed), 22)
    return {
        "tokens": draw_tokens(jax.random.fold_in(key_list[21], 71), 0),
        "input_norm_gain": jnp.clip(1.0 + 0.18 * jax.random.normal(key_list[1], (D,), jnp.float32), 0.1, 1.9),
        "input_matrix": gaussian(key_list[2], (D, HEAD_TOTAL * P_SIZE), D ** -0.5, 0.09375, ((0, 8), (1, 4))),
        "gate_matrix": gaussian(key_list[3], (D, HEAD_TOTAL * P_SIZE), D ** -0.5, 0.09375, ((0, 8), (1, 4))),
        "write_matrix": gaussian(key_list[4], (D, G * N), D ** -0.5, 0.09375, ((0, 8), (1, 4))),
        "read_matrix": gaussian(key_list[5], (D, G * N), D ** -0.5, 0.09375, ((0, 8), (1, 4))),
        "step_matrix": gaussian(key_list[6], (D, HEAD_TOTAL), D ** -0.5, 0.09375),
        "input_kernel": gaussian(key_list[7], (TAPS, HEAD_TOTAL * P_SIZE), 0.5, 3.0, ((1, 4),), jnp.float32),
        "write_kernel": gaussian(key_list[8], (TAPS, G * N), 0.5, 3.0, ((1, 4),), jnp.float32),
        "read_kernel": gaussian(key_list[9], (TAPS, G * N), 0.5, 3.0, ((1, 4),), jnp.float32),
        "step_size_bias": jnp.clip(-6.0 + 7.0 * jax.random.uniform(key_list[10], (HEAD_TOTAL,), jnp.float32) ** block_levels(key_list[10], (HEAD_TOTAL,), ((0, 4),), -0.2, 0.2), -6.0, 1.0),
        "head_decay_logs": jnp.clip(2.77 * jax.random.uniform(key_list[11], (HEAD_TOTAL,), jnp.float32) ** block_levels(key_list[11], (HEAD_TOTAL,), ((0, 4),), -0.2, 0.2), 0.0, 2.77),
        "bypass_scale": jnp.clip(0.5 + 1.0 * jax.random.uniform(key_list[12], (HEAD_TOTAL,), jnp.float32) ** block_levels(key_list[12], (HEAD_TOTAL,), ((0, 4),), -0.2, 0.2), 0.5, 1.5),
        "extra_decay_logs": draw_extra_decay_logs(jax.random.fold_in(key_list[21], 71), 0),
        "output_norm_gain": jnp.clip(1.0 + 0.18 * jax.random.normal(key_list[14], (HEAD_TOTAL * P_SIZE,), jnp.float32), 0.1, 1.9),
        "output_matrix": gaussian(key_list[15], (HEAD_TOTAL * P_SIZE, D), (HEAD_TOTAL * P_SIZE) ** -0.5, 0.09375, ((0, 4), (1, 8))),
        "cached_state_history": gaussian(key_list[16], (SEQUENCE_TOTAL, DRAFT_TOKENS + 1, HEAD_TOTAL, P_SIZE, N), 0.3, 2.0, ((0, 8), (2, 4)), jnp.float32),
        "cached_input_rows": gaussian(key_list[17], (SEQUENCE_TOTAL, DRAFT_TOKENS + TAPS - 1, HEAD_TOTAL * P_SIZE), 1.0, 6.0, ((0, 8), (2, 4))),
        "cached_write_rows": gaussian(key_list[18], (SEQUENCE_TOTAL, DRAFT_TOKENS + TAPS - 1, G * N), 1.0, 6.0, ((0, 8), (2, 4))),
        "cached_read_rows": gaussian(key_list[19], (SEQUENCE_TOTAL, DRAFT_TOKENS + TAPS - 1, G * N), 1.0, 6.0, ((0, 8), (2, 4))),
        "accepted": touch_ends(jax.random.randint(key_list[20], (SEQUENCE_TOTAL,), 0, DRAFT_TOKENS + 1), jax.random.fold_in(key_list[20], 1), 0, DRAFT_TOKENS).astype(jnp.int32),
    }


epsilon = 1e-05

def make_window(saved, fresh, accepted):
    offsets = jnp.arange(TAPS - 1, dtype=jnp.int32)
    index = (accepted[:, None] + offsets[None, :]).astype(jnp.int32)
    taken_rows = jnp.take_along_axis(saved, index[:, :, None], axis=1)
    return jnp.concatenate([taken_rows, fresh.reshape(SEQUENCE_TOTAL, DRAFT_TOKENS, -1)], axis=1)

def convolve(window, taps):
    total = jnp.zeros((window.shape[0], DRAFT_TOKENS, window.shape[2]), jnp.float32)
    for tap_index in range(TAPS):
        total = total + taps[tap_index] * window[:, tap_index:tap_index + DRAFT_TOKENS].astype(jnp.float32)
    return jax.nn.silu(total)

def reference(tokens, input_norm_gain, input_matrix, gate_matrix, write_matrix, read_matrix, step_matrix, input_kernel, write_kernel, read_kernel, step_size_bias, head_decay_logs, bypass_scale, extra_decay_logs, output_norm_gain, output_matrix, cached_state_history, cached_input_rows, cached_write_rows, cached_read_rows, accepted):
    wide_rows = tokens.astype(jnp.float32)
    inverse = lax.rsqrt(lax.optimization_barrier(jnp.sum(wide_rows * wide_rows, axis=1, keepdims=True)) / D + epsilon)
    scaled = (wide_rows * input_norm_gain).astype(jnp.bfloat16)

    def project(weight):
        return (jnp.dot(scaled, weight, preferred_element_type=jnp.float32) * inverse).astype(jnp.bfloat16)
    fresh_input = project(input_matrix)
    fresh_gate = project(gate_matrix)
    fresh_write = project(write_matrix)
    fresh_read = project(read_matrix)
    step_raw = jnp.dot(scaled, step_matrix, preferred_element_type=jnp.float32) * inverse
    next_input = make_window(cached_input_rows, fresh_input, accepted)
    next_write = make_window(cached_write_rows, fresh_write, accepted)
    next_read = make_window(cached_read_rows, fresh_read, accepted)
    conv_input = convolve(next_input, input_kernel).reshape(SEQUENCE_TOTAL, DRAFT_TOKENS, HEAD_TOTAL, P_SIZE)
    conv_write = jnp.repeat(convolve(next_write, write_kernel).reshape(SEQUENCE_TOTAL, DRAFT_TOKENS, G, N), HEAD_TOTAL // G, axis=2)
    conv_read = jnp.repeat(convolve(next_read, read_kernel).reshape(SEQUENCE_TOTAL, DRAFT_TOKENS, G, N), HEAD_TOTAL // G, axis=2)
    step_sizes = jax.nn.softplus(step_raw.reshape(SEQUENCE_TOTAL, DRAFT_TOKENS, HEAD_TOTAL) + step_size_bias)
    retain_logs = -step_sizes * jnp.exp(head_decay_logs) + extra_decay_logs.reshape(SEQUENCE_TOTAL, DRAFT_TOKENS, HEAD_TOTAL)
    carried = cached_state_history[jnp.arange(SEQUENCE_TOTAL, dtype=jnp.int32), accepted]
    states = [carried]
    outputs = []
    for position in range(DRAFT_TOKENS):
        written = (step_sizes[:, position, :, None] * conv_input[:, position])[:, :, :, None]
        carried = jnp.exp(retain_logs[:, position])[:, :, None, None] * carried + written * conv_write[:, position][:, :, None, :]
        states.append(carried)
        outputs.append(lax.optimization_barrier(jnp.sum(carried * conv_read[:, position][:, :, None, :], axis=-1)) + bypass_scale[:, None] * conv_input[:, position])
    head_out = jnp.stack(outputs, axis=1).reshape(TOKENS, HEAD_TOTAL * P_SIZE)
    gated = (head_out * jax.nn.silu(fresh_gate.astype(jnp.float32))).reshape(TOKENS, G, -1)
    gated = gated * lax.rsqrt(lax.optimization_barrier(jnp.mean(gated * gated, axis=-1, keepdims=True)) + epsilon)
    normed = (gated.reshape(TOKENS, HEAD_TOTAL * P_SIZE) * output_norm_gain).astype(jnp.bfloat16)
    span = HEAD_TOTAL * P_SIZE // N_TP
    total = jnp.zeros((TOKENS, D), jnp.float32)
    for block_index in range(N_TP):
        partial_value = jnp.dot(normed[:, block_index * span:(block_index + 1) * span], output_matrix[block_index * span:(block_index + 1) * span], preferred_element_type=jnp.float32)
        total = total + partial_value.astype(jnp.bfloat16).astype(jnp.float32)
    mixer_out = total.astype(jnp.bfloat16)
    next_states = jnp.stack(states, axis=1)
    return (mixer_out, next_states, next_input, next_write, next_read)
```

```python
import functools

import jax
import jax.numpy as jnp
from jax import lax
from jax.experimental import pallas as pl
from jax.experimental.pallas import tpu as pltpu
from jax.sharding import PartitionSpec as P

P_SIZE = 64
N = 128
TAPS = 4
DRAFT_TOKENS = 5
MESH = pl.DeviceIdType.MESH
HIGH = lax.Precision.HIGHEST
f32, bf16 = jnp.float32, jnp.bfloat16
epsilon = 1e-05


def factor(count):
    low = max(d for d in range(1, count + 1) if count % d == 0 and d * d <= count)
    return count // low, low


def remote(src, dst, send, recv, where):
    return pltpu.make_async_remote_copy(
        src_ref=src, dst_ref=dst, send_sem=send, recv_sem=recv, device_id=where, device_id_type=MESH
    )


def greet(places):
    barrier = pltpu.get_barrier_semaphore()
    for place in places:
        pl.semaphore_signal(barrier, inc=1, device_id=place, device_id_type=MESH)
    pl.semaphore_wait(barrier, len(places))


def project_kernel(
    nz, ny, own, model_width,
    tokens, gain, w_in, w_gate, w_write, w_read, step_matrix, bias, decay, extra,
    fresh_in, fresh_gate, fresh_write, fresh_read, steps_out, logs_out,
    wide, ordered, step_block, tot, *rest,
):
    pieces = 3
    send_y, recv_y, send_a, send_b, recv_a, recv_b = [
        rest[i * pieces : (i + 1) * pieces] for i in range(6)
    ]
    step_sem, sy, ry, sza, rza, szb, rzb = rest[6 * pieces :]
    me = lax.axis_index("kv")
    col = lax.axis_index("tp")
    z, y = me // ny, lax.rem(me, ny)
    width = tokens.shape[1]
    heads = bias.shape[1]
    head_rows = own - own % 16
    step_copy = pltpu.make_async_copy(
        step_matrix.at[pl.ds(pl.multiple_of(me * width, 128), width)], step_block, step_sem
    )
    step_copy.start()
    y_peers = [z * ny + lax.rem(y + d, ny) for d in range(1, ny)]
    z_peers = [lax.rem(z + d, nz) * ny + y for d in range(1, nz)]
    barrier = pltpu.get_barrier_semaphore()
    for peer in y_peers + z_peers:
        pl.semaphore_signal(barrier, inc=1, device_id={"kv": peer}, device_id_type=MESH)

    wide[...] = tokens[...].astype(f32)
    for yy in range(ny):
        for zz in range(nz):
            at = (yy * nz + zz) * own
            source = (zz * ny + yy) * own
            ordered[at : at + own] = wide[source : source + own]
    values = ordered[...]
    squares = jnp.sum(values * values, axis=1, keepdims=True)
    scaled = (values * gain[...]).astype(bf16)
    block = nz * own
    step_copy.wait()
    pick = (
        lax.broadcasted_iota(jnp.int32, (step_block.shape[1], 128), 0)
        == lax.broadcasted_iota(jnp.int32, (step_block.shape[1], 128), 1) + col * heads
    ) & (lax.broadcasted_iota(jnp.int32, (step_block.shape[1], 128), 1) < heads)
    picked = jnp.dot(
        step_block[...], pick.astype(f32).astype(bf16), preferred_element_type=f32
    ).astype(bf16)
    lane = lax.broadcasted_iota(jnp.int32, (block, 128), 1)
    sw = w_write.shape[1]

    def start_y(piece):
        copies = []
        for d in range(1, ny):
            copy = remote(
                send_y[piece].at[lax.rem(y + d, ny)], recv_y[piece].at[d - 1],
                sy.at[piece, d - 1], ry.at[piece, d - 1], {"kv": y_peers[d - 1]},
            )
            copy.start()
            copies.append(copy)
        return copies

    y_copies = []
    for piece in range(pieces):
        for yy in range(ny):
            rows = scaled[yy * block : (yy + 1) * block]
            if piece == 0:
                send_y[0][yy, :, :sw] = jnp.dot(rows, w_write[...], preferred_element_type=f32).astype(bf16)
                send_y[0][yy, :, sw : 2 * sw] = jnp.dot(rows, w_read[...], preferred_element_type=f32).astype(bf16)
                term = jnp.dot(rows, picked, preferred_element_type=f32)
                term = jnp.where(lane == heads, squares[yy * block : (yy + 1) * block], term)
                send_y[0][yy, :, 2 * sw :] = term.astype(bf16)
            else:
                weight = w_in if piece == 1 else w_gate
                send_y[piece][yy] = jnp.dot(rows, weight[...], preferred_element_type=f32).astype(bf16)
        if piece == 0:
            pl.semaphore_wait(barrier, len(y_peers) + len(z_peers))
        y_copies.append(start_y(piece))

    z_copies = []
    for piece in range(pieces):
        for copy in y_copies[piece]:
            copy.wait_recv()
        total = send_y[piece][y].astype(f32)
        for d in range(1, ny):
            total = total + recv_y[piece][d - 1].astype(f32)
        cw = total.shape[1]
        tot[:, :cw] = total
        for zz in range(nz):
            at = zz * own
            send_a[piece][zz] = tot[at : at + head_rows, :cw].astype(bf16)
            send_b[piece][zz] = tot[at + head_rows : at + own, :cw].astype(bf16)
        copies = []
        for d in range(1, nz):
            to = lax.rem(z + d, nz)
            for buf, landing, ss, rs in (
                (send_a, recv_a, sza, rza), (send_b, recv_b, szb, rzb)
            ):
                copy = remote(
                    buf[piece].at[to], landing[piece].at[d - 1],
                    ss.at[piece, d - 1], rs.at[piece, d - 1], {"kv": z_peers[d - 1]},
                )
                copy.start()
                copies.append(copy)
        z_copies.append(copies)

    inverse = None
    seqs = own // DRAFT_TOKENS
    lead = TAPS - 1
    for piece in range(pieces):
        for copy in z_copies[piece]:
            copy.wait_recv()
        total_a = send_a[piece][z].astype(f32)
        total_b = send_b[piece][z].astype(f32)
        for d in range(1, nz):
            total_a = total_a + recv_a[piece][d - 1].astype(f32)
            total_b = total_b + recv_b[piece][d - 1].astype(f32)
        cw = total_a.shape[1]
        tot[:head_rows, :cw] = total_a
        tot[head_rows:own, :cw] = total_b
        full = tot[:own, :cw]
        if piece == 0:
            tailing = full[:, 2 * sw :]
            inverse = lax.rsqrt(tailing[:, heads : heads + 1] / model_width + epsilon)
            raw = tailing[:, :heads] * inverse
            steps = jax.nn.softplus(raw + bias[...])
            logs = -steps * jnp.exp(decay[...]) + extra[...]
            fresh = (full[:, : 2 * sw] * inverse).astype(bf16).astype(f32)
            steps_out[...] = jnp.zeros_like(steps_out)
            logs_out[...] = jnp.zeros_like(logs_out)
            fresh_write[...] = jnp.zeros_like(fresh_write)
            fresh_read[...] = jnp.zeros_like(fresh_read)
            for s in range(seqs):
                cut = slice(s * DRAFT_TOKENS, (s + 1) * DRAFT_TOKENS)
                steps_out[s, :DRAFT_TOKENS] = steps[cut]
                logs_out[s, :DRAFT_TOKENS] = logs[cut]
                fresh_write[s, lead : lead + DRAFT_TOKENS] = fresh[cut, :sw]
                fresh_read[s, lead : lead + DRAFT_TOKENS] = fresh[cut, sw:]
        else:
            fresh = (full * inverse).astype(bf16).astype(f32)
            target = fresh_in if piece == 1 else fresh_gate
            first = lead if piece == 1 else 0
            target[...] = jnp.zeros_like(target)
            for s in range(seqs):
                cut = slice(s * DRAFT_TOKENS, (s + 1) * DRAFT_TOKENS)
                target[s, first : first + DRAFT_TOKENS] = fresh[cut]
    for copies in y_copies + z_copies:
        for copy in copies:
            copy.wait_send()


def state_kernel(
    group_width,
    accepted,
    fresh_in, fresh_gate, fresh_write, fresh_read, steps, logs,
    in_kernel, write_kernel, read_kernel, bypass, gain,
    saved_in, saved_write, saved_read, history,
    states, next_in, next_write, next_read, normed,
):
    taken = accepted[pl.program_id(0)]
    rows = DRAFT_TOKENS + TAPS - 1
    heads = steps.shape[2]
    width = in_kernel.shape[1]
    picks = (
        (lax.broadcasted_iota(jnp.int32, (rows, rows), 1)
         == lax.broadcasted_iota(jnp.int32, (rows, rows), 0) + taken)
        & (lax.broadcasted_iota(jnp.int32, (rows, rows), 0) < TAPS - 1)
    ).astype(f32).astype(bf16)

    def convolve(saved, fresh, taps, out):
        window = jnp.dot(picks, saved[0], preferred_element_type=f32) + fresh[0]
        out[0] = window.astype(bf16)
        total = taps[0:1] * window
        for k in range(1, TAPS):
            total = total + taps[k : k + 1] * pltpu.roll(window, rows - k, 0)
        return jax.nn.silu(total)

    x = convolve(saved_in, fresh_in, in_kernel, next_in)
    w = convolve(saved_write, fresh_write, write_kernel, next_write)
    r = convolve(saved_read, fresh_read, read_kernel, next_read)
    row = lax.broadcasted_iota(jnp.int32, (rows, heads), 0)
    log = logs[0]
    decay = jnp.zeros_like(log)
    for t in range(DRAFT_TOKENS):
        decay = decay + jnp.where(row >= t, log[t : t + 1], 0.0)
    keep = jnp.exp(decay)
    spread = (
        lax.broadcasted_iota(jnp.int32, (heads, width), 0)
        == lax.broadcasted_iota(jnp.int32, (heads, width), 1) // P_SIZE
    ).astype(f32)
    expand = functools.partial(jnp.dot, precision=HIGH, preferred_element_type=f32)
    decay_e = expand(decay, spread)
    step_x = expand(steps[0], spread) * x
    wide_row = lax.broadcasted_iota(jnp.int32, (rows, width), 0)
    direct = expand(jnp.broadcast_to(bypass[...], (rows, heads)), spread) * x
    groups = width // group_width
    per_group = group_width // P_SIZE
    gate = fresh_gate[0]
    gate = gate * jax.nn.sigmoid(gate)
    for g in range(groups):
        cut = slice(g * group_width, (g + 1) * group_width)
        wg, rg = w[:, g * N : (g + 1) * N], r[:, g * N : (g + 1) * N]
        hs = slice(g * per_group, (g + 1) * per_group)
        start = history[0, 0, hs].reshape(group_width, N)
        y = lax.dot_general(
            rg.astype(bf16), start.astype(bf16), (((1,), (1,)), ((), ())),
            preferred_element_type=f32,
        )
        dg, sg, mask_row = decay_e[:, cut], step_x[:, cut], wide_row[:, cut]
        y = y * jnp.exp(dg) + direct[:, cut]
        overlap = lax.dot_general(
            rg, wg, (((1,), (1,)), ((), ())), precision=HIGH, preferred_element_type=f32
        )
        for j in range(DRAFT_TOKENS):
            live = mask_row >= j
            fade = jnp.exp(jnp.where(live, dg - dg[j : j + 1], 0.0))
            y = y + jnp.where(live, fade * overlap[:, j : j + 1] * sg[j : j + 1], 0.0)
        gated = y * gate[:, cut]
        gated = gated * lax.rsqrt(jnp.mean(gated * gated, axis=1, keepdims=True) + epsilon)
        normed[0, :, cut] = gated * gain[:, cut]
        terms = []
        sides = []
        wide_w = jnp.concatenate([wg] * DRAFT_TOKENS, axis=1)
        lane = lax.broadcasted_iota(jnp.int32, wide_w.shape, 1) // N
        for t in range(DRAFT_TOKENS):
            live = mask_row <= t
            fade = jnp.exp(jnp.where(live, dg[t : t + 1] - dg, 0.0))
            terms.append(jnp.where(live, fade * sg, 0.0))
            sides.append(jnp.where(lane == t, wide_w, 0.0))
        left = jnp.concatenate(terms, axis=0).T.astype(bf16)
        added = jnp.dot(
            left, jnp.concatenate(sides, axis=0).astype(bf16), preferred_element_type=f32
        )
        for i in range(per_group):
            h = g * per_group + i
            own = history[0, 0, h]
            states[0, 0, h] = own
            for t in range(DRAFT_TOKENS):
                factor_th = jnp.broadcast_to(keep[t : t + 1, h : h + 1], (P_SIZE, N))
                states[0, t + 1, h] = (
                    factor_th * own
                    + added[i * P_SIZE : (i + 1) * P_SIZE, t * N : (t + 1) * N]
                )


def output_kernel(
    nz, ny, nt, own,
    normed, matrix, out,
    weight, rows_own, all_a, all_b, rows_b, send_a, send_b, recv_a, recv_b, final,
    w_sem, sz, rz, sy, ry, st, rt,
):
    me = lax.axis_index("kv")
    col = lax.axis_index("tp")
    z, y = me // ny, lax.rem(me, ny)
    w_copy = pltpu.make_async_copy(matrix, weight, w_sem)
    w_copy.start()
    head_rows = own - own % 16
    tail_rows = own - head_rows
    y_peers = [{"kv": z * ny + lax.rem(y + d, ny)} for d in range(1, ny)]
    z_peers = [{"kv": lax.rem(z + d, nz) * ny + y} for d in range(1, nz)]
    t_peers = [{"tp": lax.rem(col + d, nt)} for d in range(1, nt)]
    for s in range(own // DRAFT_TOKENS):
        rows_own[s * DRAFT_TOKENS : (s + 1) * DRAFT_TOKENS] = normed[s, :DRAFT_TOKENS]
    all_a[me] = rows_own[:head_rows].astype(bf16)
    all_b[me] = rows_own[head_rows:own].astype(bf16)
    greet(y_peers + z_peers + t_peers)

    def push(chunk, sends, recvs, place):
        pair = [
            remote(buf.at[chunk], buf.at[chunk], sends.at[i], recvs.at[i], place)
            for i, buf in enumerate((all_a, all_b))
        ]
        for copy in pair:
            copy.start()
        return pair

    z_copies = [push(me, sz.at[d], rz.at[d], z_peers[d]) for d in range(nz - 1)]
    y_sent = [push(me, sy.at[0, d], ry.at[0, d], y_peers[d]) for d in range(ny - 1)]
    for d in range(1, nz):
        for copy in z_copies[d - 1]:
            copy.wait_recv()
        chunk = lax.rem(z - d + nz, nz) * ny + y
        y_sent += [push(chunk, sy.at[d, e], ry.at[d, e], y_peers[e]) for e in range(ny - 1)]
    w_copy.wait()
    for pair in y_sent:
        for copy in pair:
            copy.wait_recv()
    for k in range(nz * ny):
        rows_b[k * tail_rows : (k + 1) * tail_rows] = all_b[k].astype(f32)
    left_a = all_a[...].reshape(nz * ny * head_rows, all_a.shape[2])
    part_a = jnp.dot(left_a, weight[...], preferred_element_type=f32)
    part_b = jnp.dot(rows_b[...].astype(bf16), weight[...], preferred_element_type=f32)
    each = nz * ny // nt
    for t in range(nt):
        send_a[t] = part_a[t * each * head_rows : (t + 1) * each * head_rows].astype(bf16)
        send_b[t] = part_b[t * each * tail_rows : (t + 1) * each * tail_rows].astype(bf16)
    t_copies = []
    for d in range(1, nt):
        to = lax.rem(col + d, nt)
        for i, (buf, landing) in enumerate(((send_a, recv_a), (send_b, recv_b))):
            copy = remote(
                buf.at[to], landing.at[d - 1], st.at[d - 1, i], rt.at[d - 1, i], t_peers[d - 1]
            )
            copy.start()
            t_copies.append(copy)
    total_a = send_a[col].astype(f32)
    total_b = send_b[col].astype(f32)
    for copy in t_copies:
        copy.wait_recv()
    for d in range(1, nt):
        total_a = total_a + recv_a[d - 1].astype(f32)
        total_b = total_b + recv_b[d - 1].astype(f32)
    for k in range(each):
        final[k * own : k * own + head_rows] = total_a[k * head_rows : (k + 1) * head_rows]
        final[k * own + head_rows : (k + 1) * own] = total_b[k * tail_rows : (k + 1) * tail_rows]
    out[...] = final[...].astype(bf16)
    for pair in z_copies + y_sent:
        for copy in pair:
            copy.wait_send()
    for copy in t_copies:
        copy.wait_send()


def per_device(
    tokens, input_norm_gain, input_matrix, gate_matrix, write_matrix, read_matrix, step_matrix,
    input_kernel, write_kernel, read_kernel, step_size_bias, head_decay_logs, bypass_scale,
    extra_decay_logs, output_norm_gain, output_matrix, cached_state_history,
    cached_input_rows, cached_write_rows, cached_read_rows, accepted,
):
    kv = lax.axis_size("kv")
    nt = lax.axis_size("tp")
    nz, ny = factor(kv)
    own = tokens.shape[0] // kv
    head_rows = own - own % 16
    tail_rows = own - head_rows
    seqs = own // DRAFT_TOKENS
    rows = DRAFT_TOKENS + TAPS - 1
    local = tokens.shape[1]
    heads = step_size_bias.shape[0]
    width = input_matrix.shape[1]
    sw = write_matrix.shape[1]
    vmem = pl.BlockSpec(memory_space=pltpu.VMEM)
    hbm = pl.BlockSpec(memory_space=pl.ANY)
    sizes = (2 * sw + 128, width, width)
    dma = pltpu.SemaphoreType.DMA
    peers = max(ny - 1, 1)
    shape = jax.ShapeDtypeStruct
    fresh_in, fresh_gate, fresh_write, fresh_read, steps, logs = pl.pallas_call(
        functools.partial(project_kernel, nz, ny, own, local * kv),
        out_shape=(
            shape((seqs, rows, width), f32), shape((seqs, rows, width), f32),
            shape((seqs, rows, sw), f32), shape((seqs, rows, sw), f32),
            shape((seqs, rows, heads), f32), shape((seqs, rows, heads), f32),
        ),
        in_specs=[vmem] * 6 + [hbm] + [vmem] * 3,
        out_specs=[vmem] * 6,
        scratch_shapes=[
            pltpu.VMEM((tokens.shape[0], local), f32),
            pltpu.VMEM((tokens.shape[0], local), f32),
            pltpu.VMEM((local, step_matrix.shape[1]), bf16),
            pltpu.VMEM((nz * own, max(sizes)), f32),
        ]
        + [pltpu.VMEM((ny, nz * own, c), bf16) for c in sizes]
        + [pltpu.VMEM((peers, nz * own, c), bf16) for c in sizes]
        + [pltpu.VMEM((nz, head_rows, c), bf16) for c in sizes]
        + [pltpu.VMEM((nz, tail_rows, c), bf16) for c in sizes]
        + [pltpu.VMEM((nz - 1, head_rows, c), bf16) for c in sizes]
        + [pltpu.VMEM((nz - 1, tail_rows, c), bf16) for c in sizes]
        + [dma(())]
        + [dma((3, peers))] * 2
        + [dma((3, nz - 1))] * 4,
        compiler_params=pltpu.CompilerParams(
            collective_id=0, has_side_effects=True, vmem_limit_bytes=40 * 2**20
        ),
    )(
        tokens, input_norm_gain[None], input_matrix, gate_matrix, write_matrix, read_matrix,
        step_matrix, step_size_bias[None], head_decay_logs[None], extra_decay_logs,
    )

    def per_seq(*dims):
        return pl.BlockSpec((1,) + dims, lambda s, acc: (s,) + (0,) * len(dims))

    def same(*dims):
        return pl.BlockSpec(dims, lambda s, acc: (0,) * len(dims))

    group_width = width // (sw // N)
    next_states, next_input, next_write, next_read, normed = pl.pallas_call(
        functools.partial(state_kernel, group_width),
        grid_spec=pltpu.PrefetchScalarGridSpec(
            num_scalar_prefetch=1,
            grid=(seqs,),
            in_specs=[
                per_seq(rows, width), per_seq(rows, width), per_seq(rows, sw), per_seq(rows, sw),
                per_seq(rows, heads), per_seq(rows, heads),
                same(TAPS, width), same(TAPS, sw), same(TAPS, sw), same(1, heads), same(1, width),
                per_seq(rows, width), per_seq(rows, sw), per_seq(rows, sw),
                pl.BlockSpec((1, 1, heads, P_SIZE, N), lambda s, acc: (s, acc[s], 0, 0, 0)),
            ],
            out_specs=[
                per_seq(DRAFT_TOKENS + 1, heads, P_SIZE, N),
                per_seq(rows, width), per_seq(rows, sw), per_seq(rows, sw), per_seq(rows, width),
            ],
        ),
        out_shape=(
            shape(cached_state_history.shape, f32),
            shape(cached_input_rows.shape, bf16),
            shape(cached_write_rows.shape, bf16),
            shape(cached_read_rows.shape, bf16),
            shape((seqs, rows, width), f32),
        ),
        compiler_params=pltpu.CompilerParams(vmem_limit_bytes=40 * 2**20),
    )(
        accepted, fresh_in, fresh_gate, fresh_write, fresh_read, steps, logs,
        input_kernel, write_kernel, read_kernel, bypass_scale[None], output_norm_gain[None],
        cached_input_rows, cached_write_rows, cached_read_rows, cached_state_history,
    )

    out_width = output_matrix.shape[1]
    each = kv // nt
    mixer_out = pl.pallas_call(
        functools.partial(output_kernel, nz, ny, nt, own),
        out_shape=shape((each * own, out_width), bf16),
        in_specs=[vmem, hbm],
        out_specs=vmem,
        scratch_shapes=[
            pltpu.VMEM(output_matrix.shape, bf16),
            pltpu.VMEM((own, width), f32),
            pltpu.VMEM((kv, head_rows, width), bf16),
            pltpu.VMEM((kv, tail_rows, width), bf16),
            pltpu.VMEM((kv * tail_rows, width), f32),
            pltpu.VMEM((nt, each * head_rows, out_width), bf16),
            pltpu.VMEM((nt, each * tail_rows, out_width), bf16),
            pltpu.VMEM((nt - 1, each * head_rows, out_width), bf16),
            pltpu.VMEM((nt - 1, each * tail_rows, out_width), bf16),
            pltpu.VMEM((each * own, out_width), f32),
            dma(()),
            dma((nz - 1, 2)), dma((nz - 1, 2)),
            dma((nz, peers, 2)), dma((nz, peers, 2)),
            dma((nt - 1, 2)), dma((nt - 1, 2)),
        ],
        compiler_params=pltpu.CompilerParams(
            collective_id=1, has_side_effects=True, vmem_limit_bytes=40 * 2**20
        ),
    )(normed, output_matrix)
    return mixer_out, next_states, next_input, next_write, next_read


def solution(mesh):
    return jax.shard_map(
        per_device,
        mesh=mesh,
        in_specs=(
            P(None, "kv"),
            P("kv"),
            P("kv", "tp"),
            P("kv", "tp"),
            P("kv", "tp"),
            P("kv", "tp"),
            P(),
            P(None, "tp"),
            P(None, "tp"),
            P(None, "tp"),
            P("tp"),
            P("tp"),
            P("tp"),
            P("kv", "tp"),
            P("tp"),
            P("tp", "kv"),
            P("kv", None, "tp", None, None),
            P("kv", None, "tp"),
            P("kv", None, "tp"),
            P("kv", None, "tp"),
            P("kv"),
        ),
        out_specs=(
            P("tp", "kv"),
            P("kv", None, "tp", None, None),
            P("kv", None, "tp"),
            P("kv", None, "tp"),
            P("kv", None, "tp"),
        ),
        check_vma=False,
    )
```

```python
import functools

import jax
import jax.numpy as jnp
from jax import lax
from jax.experimental import pallas as pl
from jax.experimental.pallas import tpu as pltpu
from jax.sharding import PartitionSpec as P

P_SIZE = 64
N = 128
TAPS = 4
DRAFT_TOKENS = 5
MESH = pl.DeviceIdType.MESH
HIGH = lax.Precision.HIGHEST
f32, bf16 = jnp.float32, jnp.bfloat16
epsilon = 1e-05
VMEM_BYTES = 67043328


def factor(count):
    low = max(d for d in range(1, count + 1) if count % d == 0 and d * d <= count)
    return count // low, low


def remote(src, dst, send, recv, where):
    return pltpu.make_async_remote_copy(
        src_ref=src, dst_ref=dst, send_sem=send, recv_sem=recv, device_id=where, device_id_type=MESH
    )


def greet(places):
    barrier = pltpu.get_barrier_semaphore()
    for place in places:
        pl.semaphore_signal(barrier, inc=1, device_id=place, device_id_type=MESH)
    pl.semaphore_wait(barrier, len(places))


def project_kernel(
    nz, ny, own, model_width,
    tokens_h, gain_h, in_h, gate_h, write_h, read_h, step_h, bias_h, decay_h, extra_h,
    fresh_in, fresh_gate, fresh_write, fresh_read, steps_out, logs_out,
    tokens, gain, w_in, w_gate, w_write, w_read, step_block, bias, decay, extra,
    wide, ordered, tot, load_sem, *rest,
):
    pieces = 5
    send_y, recv_y, send_a, send_b, recv_a, recv_b = [
        rest[i * pieces : (i + 1) * pieces] for i in range(6)
    ]
    sy, ry, sza, rza, szb, rzb = rest[6 * pieces :]
    me = lax.axis_index("kv")
    col = lax.axis_index("tp")
    z, y = me // ny, lax.rem(me, ny)
    width = tokens.shape[1]
    heads = bias.shape[1]
    head_rows = own - own % 16
    half = w_in.shape[1] // 2
    step_cut = step_h.at[:, pl.ds(pl.multiple_of(me * width, 128), width)]
    loads = [
        pltpu.make_async_copy(source, target, load_sem.at[i])
        for i, (source, target) in enumerate((
            (tokens_h, tokens), (gain_h, gain), (step_cut, step_block), (write_h, w_write),
            (read_h, w_read), (in_h, w_in), (gate_h, w_gate), (bias_h, bias),
            (decay_h, decay), (extra_h, extra),
        ))
    ]
    for load in loads:
        load.start()
    y_peers = [z * ny + lax.rem(y + d, ny) for d in range(1, ny)]
    z_peers = [lax.rem(z + d, nz) * ny + y for d in range(1, nz)]
    barrier = pltpu.get_barrier_semaphore()
    for peer in y_peers + z_peers:
        pl.semaphore_signal(barrier, inc=1, device_id={"kv": peer}, device_id_type=MESH)

    loads[0].wait()
    loads[1].wait()
    wide[...] = tokens[...].astype(f32)
    for yy in range(ny):
        for zz in range(nz):
            at = (yy * nz + zz) * own
            source = (zz * ny + yy) * own
            ordered[at : at + own] = wide[source : source + own]
    values = ordered[...]
    squares = jnp.sum(values * values, axis=1, keepdims=True)
    scaled = (values * gain[...]).astype(bf16)
    block = nz * own
    for load in loads[2:5]:
        load.wait()
    picked_row = lax.broadcasted_iota(jnp.int32, (128, step_block.shape[0]), 0)
    pick = (
        lax.broadcasted_iota(jnp.int32, (128, step_block.shape[0]), 1) == picked_row + col * heads
    ) & (picked_row < heads)
    picked = jnp.dot(
        pick.astype(f32).astype(bf16), step_block[...], preferred_element_type=f32
    ).astype(bf16)
    lane = lax.broadcasted_iota(jnp.int32, (block, 128), 1)
    sw = w_write.shape[1]

    def start_y(piece):
        copies = []
        for d in range(1, ny):
            copy = remote(
                send_y[piece].at[lax.rem(y + d, ny)], recv_y[piece].at[d - 1],
                sy.at[piece, d - 1], ry.at[piece, d - 1], {"kv": y_peers[d - 1]},
            )
            copy.start()
            copies.append(copy)
        return copies

    y_copies = []
    for piece in range(pieces):
        if piece == 1:
            loads[5].wait()
        if piece == 3:
            loads[6].wait()
        for yy in range(ny):
            rows = scaled[yy * block : (yy + 1) * block]
            if piece == 0:
                send_y[0][yy, :, :sw] = jnp.dot(rows, w_write[...], preferred_element_type=f32).astype(bf16)
                send_y[0][yy, :, sw : 2 * sw] = jnp.dot(rows, w_read[...], preferred_element_type=f32).astype(bf16)
                term = lax.dot_general(
                    rows, picked, (((1,), (1,)), ((), ())), preferred_element_type=f32
                )
                term = jnp.where(lane == heads, squares[yy * block : (yy + 1) * block], term)
                send_y[0][yy, :, 2 * sw :] = term.astype(bf16)
            else:
                weight = w_in if piece < 3 else w_gate
                first = (piece - 1) % 2 * half
                send_y[piece][yy] = jnp.dot(
                    rows, weight[:, first : first + half], preferred_element_type=f32
                ).astype(bf16)
        if piece == 0:
            pl.semaphore_wait(barrier, len(y_peers) + len(z_peers))
        y_copies.append(start_y(piece))

    z_copies = []
    for piece in range(pieces):
        for copy in y_copies[piece]:
            copy.wait_recv()
        total = send_y[piece][y].astype(f32)
        for d in range(1, ny):
            total = total + recv_y[piece][d - 1].astype(f32)
        cw = total.shape[1]
        tot[:, :cw] = total
        for zz in range(nz):
            at = zz * own
            send_a[piece][zz] = tot[at : at + head_rows, :cw].astype(bf16)
            send_b[piece][zz] = tot[at + head_rows : at + own, :cw].astype(bf16)
        copies = []
        for d in range(1, nz):
            to = lax.rem(z + d, nz)
            for buf, landing, ss, rs in (
                (send_a, recv_a, sza, rza), (send_b, recv_b, szb, rzb)
            ):
                copy = remote(
                    buf[piece].at[to], landing[piece].at[d - 1],
                    ss.at[piece, d - 1], rs.at[piece, d - 1], {"kv": z_peers[d - 1]},
                )
                copy.start()
                copies.append(copy)
        z_copies.append(copies)

    for load in loads[7:]:
        load.wait()
    inverse = None
    seqs = own // DRAFT_TOKENS
    lead = TAPS - 1
    for piece in range(pieces):
        for copy in z_copies[piece]:
            copy.wait_recv()
        total_a = send_a[piece][z].astype(f32)
        total_b = send_b[piece][z].astype(f32)
        for d in range(1, nz):
            total_a = total_a + recv_a[piece][d - 1].astype(f32)
            total_b = total_b + recv_b[piece][d - 1].astype(f32)
        cw = total_a.shape[1]
        tot[:head_rows, :cw] = total_a
        tot[head_rows:own, :cw] = total_b
        full = tot[:own, :cw]
        if piece == 0:
            tailing = full[:, 2 * sw :]
            inverse = lax.rsqrt(tailing[:, heads : heads + 1] / model_width + epsilon)
            raw = tailing[:, :heads] * inverse
            steps = jax.nn.softplus(raw + bias[...])
            same_row = lax.broadcasted_iota(jnp.int32, (own, own), 0) == lax.broadcasted_iota(
                jnp.int32, (own, own), 1
            )
            added_logs = lax.dot_general(
                same_row.astype(f32), extra[...], (((1,), (1,)), ((), ())),
                precision=HIGH, preferred_element_type=f32,
            )
            logs = -steps * jnp.exp(decay[...]) + added_logs
            fresh = (full[:, : 2 * sw] * inverse).astype(bf16).astype(f32)
            steps_out[...] = jnp.zeros_like(steps_out)
            logs_out[...] = jnp.zeros_like(logs_out)
            fresh_write[...] = jnp.zeros_like(fresh_write)
            fresh_read[...] = jnp.zeros_like(fresh_read)
            for s in range(seqs):
                cut = slice(s * DRAFT_TOKENS, (s + 1) * DRAFT_TOKENS)
                steps_out[s, :DRAFT_TOKENS] = steps[cut]
                logs_out[s, :DRAFT_TOKENS] = logs[cut]
                fresh_write[s, lead : lead + DRAFT_TOKENS] = fresh[cut, :sw]
                fresh_read[s, lead : lead + DRAFT_TOKENS] = fresh[cut, sw:]
        else:
            fresh = (full * inverse).astype(bf16).astype(f32)
            target = fresh_in if piece < 3 else fresh_gate
            first = lead if piece < 3 else 0
            if piece % 2 == 1:
                target[...] = jnp.zeros_like(target)
            columns = slice((piece - 1) % 2 * half, (piece - 1) % 2 * half + half)
            for s in range(seqs):
                cut = slice(s * DRAFT_TOKENS, (s + 1) * DRAFT_TOKENS)
                target[s, first : first + DRAFT_TOKENS, columns] = fresh[cut]
    for copies in y_copies + z_copies:
        for copy in copies:
            copy.wait_send()


def state_kernel(
    group_width,
    accepted,
    fresh_in, fresh_gate, fresh_write, fresh_read, steps, logs,
    in_kernel, write_kernel, read_kernel, bypass, gain,
    saved_in, saved_write, saved_read, history,
    states, next_in, next_write, next_read, normed,
):
    taken = accepted[pl.program_id(0)]
    rows = DRAFT_TOKENS + TAPS - 1
    heads = steps.shape[2]
    width = in_kernel.shape[1]
    picks = (
        (lax.broadcasted_iota(jnp.int32, (rows, rows), 1)
         == lax.broadcasted_iota(jnp.int32, (rows, rows), 0) + taken)
        & (lax.broadcasted_iota(jnp.int32, (rows, rows), 0) < TAPS - 1)
    ).astype(f32).astype(bf16)

    def convolve(saved, fresh, taps, out):
        window = jnp.dot(picks, saved[0], preferred_element_type=f32) + fresh[0]
        out[0] = window.astype(bf16)
        total = taps[0:1] * window
        for k in range(1, TAPS):
            total = total + taps[k : k + 1] * pltpu.roll(window, rows - k, 0)
        return jax.nn.silu(total)

    x = convolve(saved_in, fresh_in, in_kernel, next_in)
    w = convolve(saved_write, fresh_write, write_kernel, next_write)
    r = convolve(saved_read, fresh_read, read_kernel, next_read)
    row = lax.broadcasted_iota(jnp.int32, (rows, heads), 0)
    log = logs[0]
    decay = jnp.zeros_like(log)
    for t in range(DRAFT_TOKENS):
        decay = decay + jnp.where(row >= t, log[t : t + 1], 0.0)
    keep = jnp.exp(decay)
    spread = (
        lax.broadcasted_iota(jnp.int32, (heads, width), 0)
        == lax.broadcasted_iota(jnp.int32, (heads, width), 1) // P_SIZE
    ).astype(f32)
    expand = functools.partial(jnp.dot, precision=HIGH, preferred_element_type=f32)
    decay_e = expand(decay, spread)
    step_x = expand(steps[0], spread) * x
    wide_row = lax.broadcasted_iota(jnp.int32, (rows, width), 0)
    direct = expand(jnp.broadcast_to(bypass[...], (rows, heads)), spread) * x
    groups = width // group_width
    per_group = group_width // P_SIZE
    gate = fresh_gate[0]
    gate = gate * jax.nn.sigmoid(gate)
    for g in range(groups):
        cut = slice(g * group_width, (g + 1) * group_width)
        wg, rg = w[:, g * N : (g + 1) * N], r[:, g * N : (g + 1) * N]
        hs = slice(g * per_group, (g + 1) * per_group)
        start = history[0, 0, hs].reshape(group_width, N)
        y = lax.dot_general(
            rg.astype(bf16), start.astype(bf16), (((1,), (1,)), ((), ())),
            preferred_element_type=f32,
        )
        dg, sg, mask_row = decay_e[:, cut], step_x[:, cut], wide_row[:, cut]
        y = y * jnp.exp(dg) + direct[:, cut]
        overlap = lax.dot_general(
            rg, wg, (((1,), (1,)), ((), ())), precision=HIGH, preferred_element_type=f32
        )
        for j in range(DRAFT_TOKENS):
            live = mask_row >= j
            fade = jnp.exp(jnp.where(live, dg - dg[j : j + 1], 0.0))
            y = y + jnp.where(live, fade * overlap[:, j : j + 1] * sg[j : j + 1], 0.0)
        gated = y * gate[:, cut]
        gated = gated * lax.rsqrt(jnp.mean(gated * gated, axis=1, keepdims=True) + epsilon)
        normed[0, :, cut] = gated * gain[:, cut]
        terms = []
        sides = []
        wide_w = jnp.concatenate([wg] * DRAFT_TOKENS, axis=1)
        lane = lax.broadcasted_iota(jnp.int32, wide_w.shape, 1) // N
        for t in range(DRAFT_TOKENS):
            live = mask_row <= t
            fade = jnp.exp(jnp.where(live, dg[t : t + 1] - dg, 0.0))
            terms.append(jnp.where(live, fade * sg, 0.0))
            sides.append(jnp.where(lane == t, wide_w, 0.0))
        left = jnp.concatenate(terms, axis=0).T.astype(bf16)
        added = jnp.dot(
            left, jnp.concatenate(sides, axis=0).astype(bf16), preferred_element_type=f32
        )
        for i in range(per_group):
            h = g * per_group + i
            own = history[0, 0, h]
            states[0, 0, h] = own
            for t in range(DRAFT_TOKENS):
                factor_th = jnp.broadcast_to(keep[t : t + 1, h : h + 1], (P_SIZE, N))
                states[0, t + 1, h] = (
                    factor_th * own
                    + added[i * P_SIZE : (i + 1) * P_SIZE, t * N : (t + 1) * N]
                )


def output_kernel(
    nz, ny, nt, own,
    normed, matrix, out,
    weight, rows_own, all_a, all_b, rows_b, send_a, send_b, recv_a, recv_b, final,
    w_sem, sz, rz, sy, ry, st, rt,
):
    me = lax.axis_index("kv")
    col = lax.axis_index("tp")
    z, y = me // ny, lax.rem(me, ny)
    w_copy = pltpu.make_async_copy(matrix, weight, w_sem)
    w_copy.start()
    head_rows = own - own % 16
    tail_rows = own - head_rows
    y_peers = [{"kv": z * ny + lax.rem(y + d, ny)} for d in range(1, ny)]
    z_peers = [{"kv": lax.rem(z + d, nz) * ny + y} for d in range(1, nz)]
    t_peers = [{"tp": lax.rem(col + d, nt)} for d in range(1, nt)]
    for s in range(own // DRAFT_TOKENS):
        rows_own[s * DRAFT_TOKENS : (s + 1) * DRAFT_TOKENS] = normed[s, :DRAFT_TOKENS]
    all_a[me] = rows_own[:head_rows].astype(bf16)
    all_b[me] = rows_own[head_rows:own].astype(bf16)
    greet(y_peers + z_peers + t_peers)

    def push(chunk, sends, recvs, place):
        pair = [
            remote(buf.at[chunk], buf.at[chunk], sends.at[i], recvs.at[i], place)
            for i, buf in enumerate((all_a, all_b))
        ]
        for copy in pair:
            copy.start()
        return pair

    z_copies = [push(me, sz.at[d], rz.at[d], z_peers[d]) for d in range(nz - 1)]
    y_sent = [push(me, sy.at[0, d], ry.at[0, d], y_peers[d]) for d in range(ny - 1)]
    for d in range(1, nz):
        for copy in z_copies[d - 1]:
            copy.wait_recv()
        chunk = lax.rem(z - d + nz, nz) * ny + y
        y_sent += [push(chunk, sy.at[d, e], ry.at[d, e], y_peers[e]) for e in range(ny - 1)]
    w_copy.wait()
    for pair in y_sent:
        for copy in pair:
            copy.wait_recv()
    for k in range(nz * ny):
        rows_b[k * tail_rows : (k + 1) * tail_rows] = all_b[k].astype(f32)
    left_a = all_a[...].reshape(nz * ny * head_rows, all_a.shape[2])
    part_a = jnp.dot(left_a, weight[...], preferred_element_type=f32)
    part_b = jnp.dot(rows_b[...].astype(bf16), weight[...], preferred_element_type=f32)
    each = nz * ny // nt
    for t in range(nt):
        send_a[t] = part_a[t * each * head_rows : (t + 1) * each * head_rows].astype(bf16)
        send_b[t] = part_b[t * each * tail_rows : (t + 1) * each * tail_rows].astype(bf16)
    t_copies = []
    for d in range(1, nt):
        to = lax.rem(col + d, nt)
        for i, (buf, landing) in enumerate(((send_a, recv_a), (send_b, recv_b))):
            copy = remote(
                buf.at[to], landing.at[d - 1], st.at[d - 1, i], rt.at[d - 1, i], t_peers[d - 1]
            )
            copy.start()
            t_copies.append(copy)
    total_a = send_a[col].astype(f32)
    total_b = send_b[col].astype(f32)
    for copy in t_copies:
        copy.wait_recv()
    for d in range(1, nt):
        total_a = total_a + recv_a[d - 1].astype(f32)
        total_b = total_b + recv_b[d - 1].astype(f32)
    for k in range(each):
        final[k * own : k * own + head_rows] = total_a[k * head_rows : (k + 1) * head_rows]
        final[k * own + head_rows : (k + 1) * own] = total_b[k * tail_rows : (k + 1) * tail_rows]
    out[...] = final[...].astype(bf16)
    for pair in z_copies + y_sent:
        for copy in pair:
            copy.wait_send()
    for copy in t_copies:
        copy.wait_send()


def per_device(
    tokens, input_norm_gain, input_matrix, gate_matrix, write_matrix, read_matrix, step_matrix,
    input_kernel, write_kernel, read_kernel, step_size_bias, head_decay_logs, bypass_scale,
    extra_decay_logs, output_norm_gain, output_matrix, cached_state_history,
    cached_input_rows, cached_write_rows, cached_read_rows, accepted,
):
    kv = lax.axis_size("kv")
    nt = lax.axis_size("tp")
    nz, ny = factor(kv)
    own = tokens.shape[0] // kv
    head_rows = own - own % 16
    tail_rows = own - head_rows
    seqs = own // DRAFT_TOKENS
    rows = DRAFT_TOKENS + TAPS - 1
    local = tokens.shape[1]
    heads = step_size_bias.shape[0]
    width = input_matrix.shape[1]
    sw = write_matrix.shape[1]
    vmem = pl.BlockSpec(memory_space=pltpu.VMEM)
    hbm = pl.BlockSpec(memory_space=pl.ANY)
    sizes = (2 * sw + 128,) + (width // 2,) * 4
    dma = pltpu.SemaphoreType.DMA
    peers = max(ny - 1, 1)
    shape = jax.ShapeDtypeStruct
    fresh_in, fresh_gate, fresh_write, fresh_read, steps, logs = pl.pallas_call(
        functools.partial(project_kernel, nz, ny, own, local * kv),
        out_shape=(
            shape((seqs, rows, width), f32), shape((seqs, rows, width), f32),
            shape((seqs, rows, sw), f32), shape((seqs, rows, sw), f32),
            shape((seqs, rows, heads), f32), shape((seqs, rows, heads), f32),
        ),
        in_specs=[hbm] * 10,
        out_specs=[vmem] * 6,
        scratch_shapes=[
            pltpu.VMEM(tokens.shape, bf16),
            pltpu.VMEM((1, local), f32),
            pltpu.VMEM((local, width), bf16),
            pltpu.VMEM((local, width), bf16),
            pltpu.VMEM((local, sw), bf16),
            pltpu.VMEM((local, sw), bf16),
            pltpu.VMEM((step_matrix.shape[1], local), bf16),
            pltpu.VMEM((1, heads), f32),
            pltpu.VMEM((1, heads), f32),
            pltpu.VMEM((heads, own), f32),
            pltpu.VMEM((tokens.shape[0], local), f32),
            pltpu.VMEM((tokens.shape[0], local), f32),
            pltpu.VMEM((nz * own, max(sizes)), f32),
            dma((10,)),
        ]
        + [pltpu.VMEM((ny, nz * own, c), bf16) for c in sizes]
        + [pltpu.VMEM((peers, nz * own, c), bf16) for c in sizes]
        + [pltpu.VMEM((nz, head_rows, c), bf16) for c in sizes]
        + [pltpu.VMEM((nz, tail_rows, c), bf16) for c in sizes]
        + [pltpu.VMEM((nz - 1, head_rows, c), bf16) for c in sizes]
        + [pltpu.VMEM((nz - 1, tail_rows, c), bf16) for c in sizes]
        + [dma((5, peers))] * 2
        + [dma((5, nz - 1))] * 4,
        compiler_params=pltpu.CompilerParams(
            collective_id=0, has_side_effects=True, vmem_limit_bytes=VMEM_BYTES
        ),
    )(
        tokens, input_norm_gain[None], input_matrix, gate_matrix, write_matrix, read_matrix,
        step_matrix.T, step_size_bias[None], head_decay_logs[None], extra_decay_logs.T,
    )

    def per_seq(*dims):
        return pl.BlockSpec((1,) + dims, lambda s, acc: (s,) + (0,) * len(dims))

    def same(*dims):
        return pl.BlockSpec(dims, lambda s, acc: (0,) * len(dims))

    group_width = width // (sw // N)
    next_states, next_input, next_write, next_read, normed = pl.pallas_call(
        functools.partial(state_kernel, group_width),
        grid_spec=pltpu.PrefetchScalarGridSpec(
            num_scalar_prefetch=1,
            grid=(seqs,),
            in_specs=[
                per_seq(rows, width), per_seq(rows, width), per_seq(rows, sw), per_seq(rows, sw),
                per_seq(rows, heads), per_seq(rows, heads),
                same(TAPS, width), same(TAPS, sw), same(TAPS, sw), same(1, heads), same(1, width),
                per_seq(rows, width), per_seq(rows, sw), per_seq(rows, sw),
                pl.BlockSpec((1, 1, heads, P_SIZE, N), lambda s, acc: (s, acc[s], 0, 0, 0)),
            ],
            out_specs=[
                per_seq(DRAFT_TOKENS + 1, heads, P_SIZE, N),
                per_seq(rows, width), per_seq(rows, sw), per_seq(rows, sw), per_seq(rows, width),
            ],
        ),
        out_shape=(
            shape(cached_state_history.shape, f32),
            shape(cached_input_rows.shape, bf16),
            shape(cached_write_rows.shape, bf16),
            shape(cached_read_rows.shape, bf16),
            shape((seqs, rows, width), f32),
        ),
        compiler_params=pltpu.CompilerParams(vmem_limit_bytes=VMEM_BYTES),
    )(
        accepted, fresh_in, fresh_gate, fresh_write, fresh_read, steps, logs,
        input_kernel, write_kernel, read_kernel, bypass_scale[None], output_norm_gain[None],
        cached_input_rows, cached_write_rows, cached_read_rows, cached_state_history,
    )

    out_width = output_matrix.shape[1]
    each = kv // nt
    mixer_out = pl.pallas_call(
        functools.partial(output_kernel, nz, ny, nt, own),
        out_shape=shape((each * own, out_width), bf16),
        in_specs=[vmem, hbm],
        out_specs=vmem,
        scratch_shapes=[
            pltpu.VMEM(output_matrix.shape, bf16),
            pltpu.VMEM((own, width), f32),
            pltpu.VMEM((kv, head_rows, width), bf16),
            pltpu.VMEM((kv, tail_rows, width), bf16),
            pltpu.VMEM((kv * tail_rows, width), f32),
            pltpu.VMEM((nt, each * head_rows, out_width), bf16),
            pltpu.VMEM((nt, each * tail_rows, out_width), bf16),
            pltpu.VMEM((nt - 1, each * head_rows, out_width), bf16),
            pltpu.VMEM((nt - 1, each * tail_rows, out_width), bf16),
            pltpu.VMEM((each * own, out_width), f32),
            dma(()),
            dma((nz - 1, 2)), dma((nz - 1, 2)),
            dma((nz, peers, 2)), dma((nz, peers, 2)),
            dma((nt - 1, 2)), dma((nt - 1, 2)),
        ],
        compiler_params=pltpu.CompilerParams(
            collective_id=1, has_side_effects=True, vmem_limit_bytes=VMEM_BYTES
        ),
    )(normed, output_matrix)
    return mixer_out, next_states, next_input, next_write, next_read


def solution(mesh):
    return jax.shard_map(
        per_device,
        mesh=mesh,
        in_specs=(
            P(None, "kv"),
            P("kv"),
            P("kv", "tp"),
            P("kv", "tp"),
            P("kv", "tp"),
            P("kv", "tp"),
            P(),
            P(None, "tp"),
            P(None, "tp"),
            P(None, "tp"),
            P("tp"),
            P("tp"),
            P("tp"),
            P("kv", "tp"),
            P("tp"),
            P("tp", "kv"),
            P("kv", None, "tp", None, None),
            P("kv", None, "tp"),
            P("kv", None, "tp"),
            P("kv", None, "tp"),
            P("kv"),
        ),
        out_specs=(
            P("tp", "kv"),
            P("kv", None, "tp", None, None),
            P("kv", None, "tp"),
            P("kv", None, "tp"),
            P("kv", None, "tp"),
        ),
        check_vma=False,
    )
```
